32 devices in a mesh: sp: 16 (over z, y, x), tp: 2 (over core).
Axes of the slice: x: 2, y: 2, z: 4, core: 2. Of those that a mesh axis runs over, the one named last changes fastest.
Arguments:
- skip_stream_entering: bfloat16 [1024, 2048], P('sp'), may hold values from -6 to 6
- reading_vectors: bfloat16 [1024, 1024], P('sp', 'tp'), may hold values from -6 to 6
- blender_lookup_labels: bfloat16 [1024, 1024], P('sp', 'tp'), may hold values from -6 to 6
- blender_payloads: bfloat16 [1024, 1024], P('sp', 'tp'), may hold values from -6 to 6
- blender_result_valve: bfloat16 [1024, 1024], P('sp', 'tp'), may hold values from -6 to 6
- fading_logits: bfloat16 [2, 1024, 1024], P(None, 'sp', 'tp'), as said below
- amend_speed_logits: bfloat16 [2, 1024, 1024], P(None, 'sp', 'tp'), as said below
- extra_log_fades: float32 [2, 16, 1024], P(None, 'tp', 'sp'), may hold values from -3 to 0
- present_reward_factors: float32 [1024], P('tp'), may hold values from -1.2 to 1.2
- attender_scaling_vector: float32 [1024], P('tp'), may hold values from 0.1 to 1.9
- blender_result_projector: bfloat16 [1024, 2048], P('tp'), may hold values from -0.1875 to 0.1875
- blender_scaling_vector: float32 [2048], replicated, may hold values from 0.1 to 1.9
- perceptron_valve_factors: bfloat16 [2048, 5632], P('sp', 'tp'), may hold values from -0.125 to 0.125
- perceptron_widen_factors: bfloat16 [2048, 5632], P('sp', 'tp'), may hold values from -0.125 to 0.125
- perceptron_shrink_factors: bfloat16 [5632, 2048], P('tp', 'sp'), may hold values from -0.078125 to 0.078125
- closing_scaling_vector: float32 [2048], replicated, may hold values from 0.1 to 1.9
Outputs:
- result: bfloat16 [1024, 2048], P(('sp', 'tp'))
The draws below stay inside these ranges and needn't reach their ends.
Inputs may be any that keep to these rules, and one draw needn't show every extreme that they name: `fading_logits`: decay pre-activations. `amend_speed_logits`: correction-rate pre-activations.
All inputs are finite; a program needn't handle non-finite values.
Results may differ from the reference program's by a relative error of at most 0.02.
Values may be sent and summed in bfloat16 or wider, within the bound.
A program may use at most 128 MiB of HBM per device.

```python
import math
import jax
import jax.numpy as jnp
from jax import lax

D = 2048
FF = 5632
HEADS = 16
HEAD = 64
TOK_DEV = 64
STRING_LENGTH = 1024
BLENDER_WIDTH = 1024
N_TP = 2


def head_classes(key):
    picked = jax.random.uniform(jax.random.fold_in(key, 101), (2, HEADS), jnp.float32)
    slow_share = 0.5
    mixed_index = jax.random.randint(jax.random.fold_in(key, 102), (2,), 0, HEADS)
    mixed = (jnp.arange(HEADS, dtype=jnp.int32)[None, :] == mixed_index[:, None]).astype(jnp.float32)
    slow = (picked < slow_share).astype(jnp.float32) * (1.0 - mixed)
    return (slow, mixed)


def fast_blocks(key):
    block_count = STRING_LENGTH // TOK_DEV
    phase = jax.random.randint(jax.random.fold_in(key, 103), (2,), 0, 8)
    place = (jnp.arange(block_count, dtype=jnp.int32)[None, :] + phase[:, None]) % 8
    extra = jax.random.randint(jax.random.fold_in(key, 104), (2, block_count), 0, 2)
    return jnp.where(place == 4, 1.0, jnp.where(place == 0, extra.astype(jnp.float32), 0.0))


def draw_fading_logits(key, part):
    slow, mixed = head_classes(key)
    block_count = STRING_LENGTH // TOK_DEV
    quick = fast_blocks(key)
    slow_now = slow[:, None, :] + mixed[:, None, :] * (1.0 - quick[:, :, None])
    slow_now = jnp.broadcast_to(slow_now[:, :, None, :], (2, block_count, TOK_DEV, HEADS)).reshape(2, STRING_LENGTH, HEADS)
    slow_cols = jnp.repeat(slow_now, HEAD, axis=2)
    base_vals = slow_cols * (-math.log(STRING_LENGTH) - 0.2) + (1.0 - slow_cols) * -4.0
    offsets = jax.random.uniform(jax.random.fold_in(key, 11), (2, block_count, 1, HEADS), jnp.float32, -0.7, 0.7)
    offsets = jnp.broadcast_to(offsets, (2, block_count, TOK_DEV, HEADS)).reshape(2, STRING_LENGTH, HEADS)
    offsets = jnp.repeat(offsets, HEAD, axis=2)
    noise_vals = jnp.clip(0.5 * jax.random.normal(jax.random.fold_in(key, 12), (2, STRING_LENGTH, BLENDER_WIDTH), jnp.float32), -1.5, 1.5)
    return (base_vals + offsets + noise_vals).astype(jnp.bfloat16)


def draw_amend_speed_logits(key, part):
    slow, mixed = head_classes(key)
    slow_cols = jnp.repeat(slow + mixed, HEAD, axis=1)
    base_vals = slow_cols * math.log(32.0 / STRING_LENGTH)
    noise_vals = jnp.clip(0.7 * jax.random.normal(jax.random.fold_in(key, 21), (2, STRING_LENGTH, BLENDER_WIDTH), jnp.float32), -2.0, 2.0)
    return (base_vals[:, None, :] + noise_vals).astype(jnp.bfloat16)


def draw_extra_log_fades(key, part):
    spots = jax.random.randint(jax.random.fold_in(key, 31), (2, HEADS, 6), 0, STRING_LENGTH)
    depths = jnp.log(jax.random.uniform(jax.random.fold_in(key, 32), (2, HEADS, 6), jnp.float32, 0.5, 0.8))
    places = jnp.arange(STRING_LENGTH, dtype=jnp.int32)
    hits = (spots[..., None] == places).astype(jnp.float32)
    return jnp.einsum('dhb,dhbt->dht', depths, hits)


def levels(stream_key, dims, pieces, least, top_value):
    def one(dim, shards_of):
        draws = jax.random.uniform(jax.random.fold_in(jax.random.fold_in(stream_key, 6), dim), (shards_of,), jnp.float32, least / len(pieces), top_value / len(pieces))
        return jnp.repeat(jnp.exp(draws), dims[dim] // shards_of).reshape((-1,) + (1,) * (len(dims) - dim - 1))

    factor_of = one(*pieces[0])
    for cut in pieces[1:]:
        factor_of = factor_of * one(*cut)
    return factor_of


def scatter_about(key, dims, scale, most, split=(), kind=jnp.bfloat16):
    level = levels(key, dims, split, -0.22, 0.18) if split else 1.0
    values = jax.random.normal(key, dims, jnp.float32) * scale * level
    return jnp.minimum(jnp.maximum(values, -most), most).astype(kind)


def setup_inputs(seed: int = 0) -> dict:
    key_list = jax.random.split(jax.random.key(seed), 17)
    return {
        "skip_stream_entering": scatter_about(key_list[0], (STRING_LENGTH, D), 1.0, 6.0, ((0, 16),)),
        "reading_vectors": scatter_about(key_list[1], (STRING_LENGTH, BLENDER_WIDTH), 1.0, 6.0, ((0, 16), (1, 2))),
        "blender_lookup_labels": scatter_about(key_list[2], (STRING_LENGTH, BLENDER_WIDTH), 1.0, 6.0, ((0, 16), (1, 2))),
        "blender_payloads": scatter_about(key_list[3], (STRING_LENGTH, BLENDER_WIDTH), 1.0, 6.0, ((0, 16), (1, 2))),
        "blender_result_valve": scatter_about(key_list[4], (STRING_LENGTH, BLENDER_WIDTH), 1.0, 6.0, ((0, 16), (1, 2))),
        "fading_logits": draw_fading_logits(jax.random.fold_in(key_list[16], 71), 0),
        "amend_speed_logits": draw_amend_speed_logits(jax.random.fold_in(key_list[16], 71), 0),
        "extra_log_fades": draw_extra_log_fades(jax.random.fold_in(key_list[16], 71), 0),
        "present_reward_factors": scatter_about(key_list[8], (BLENDER_WIDTH,), 0.2, 1.2, ((0, 2),), jnp.float32),
        "attender_scaling_vector": jnp.clip(1.0 + 0.18 * jax.random.normal(key_list[9], (BLENDER_WIDTH,), jnp.float32), 0.1, 1.9),
        "blender_result_projector": scatter_about(key_list[10], (BLENDER_WIDTH, D), BLENDER_WIDTH ** -0.5, 0.1875, ((0, 2),)),
        "blender_scaling_vector": jnp.clip(1.0 + 0.18 * jax.random.normal(key_list[11], (D,), jnp.float32), 0.1, 1.9),
        "perceptron_valve_factors": scatter_about(key_list[12], (D, FF), D ** -0.5, 0.125, ((0, 16), (1, 2))),
        "perceptron_widen_factors": scatter_about(key_list[13], (D, FF), D ** -0.5, 0.125, ((0, 16), (1, 2))),
        "perceptron_shrink_factors": scatter_about(key_list[14], (FF, D), FF ** -0.5, 0.078125, ((0, 2), (1, 16))),
        "closing_scaling_vector": jnp.clip(1.0 + 0.18 * jax.random.normal(key_list[15], (D,), jnp.float32), 0.1, 1.9),
    }


RESIDUAL_SCALE = 2.0 ** 0.25
NORM_EPS = 1e-05
GROUP_EPS = 0.00064
KEY_EPS = 1e-06
PRECISE = lax.Precision.HIGHEST

def layer_norm(summand, gain_vec):
    center = lax.optimization_barrier(jnp.mean(summand, -1, keepdims=True))
    spread = lax.optimization_barrier(jnp.mean(jnp.square(summand - center), -1, keepdims=True))
    return (summand - center) * lax.rsqrt(spread + NORM_EPS) * gain_vec

def wire_round(tensor):
    return lax.optimization_barrier(tensor.astype(jnp.bfloat16)).astype(jnp.float32)

def direction_scan(entire_asking_lines, decays, stored_label_lines, payload_line_slab, erase_keys, refills):

    def advance(state_mat, inputs):
        query_vec, decay_vec, write_key, value_vec, erase_vec, refill_vec = inputs
        erased = jnp.einsum('hij,hj->hi', state_mat, erase_vec, precision=PRECISE)
        state_mat = state_mat * decay_vec[:, None, :] + erased[:, :, None] * refill_vec[:, None, :] + value_vec[:, :, None] * write_key[:, None, :]
        return (state_mat, jnp.einsum('hij,hj->hi', state_mat, query_vec, precision=PRECISE))
    start_state = jnp.zeros((HEADS, HEAD, HEAD), jnp.float32)
    _, outputs = lax.scan(advance, start_state, (entire_asking_lines, decays, stored_label_lines, payload_line_slab, erase_keys, refills))
    return outputs

def reference(skip_stream_entering, reading_vectors, blender_lookup_labels, blender_payloads, blender_result_valve, fading_logits, amend_speed_logits, extra_log_fades, present_reward_factors, attender_scaling_vector, blender_result_projector, blender_scaling_vector, perceptron_valve_factors, perceptron_widen_factors, perceptron_shrink_factors, closing_scaling_vector):

    def split_attenders(tensor):
        return tensor.reshape(tensor.shape[:-1] + (HEADS, HEAD))

    def flipped(tensor):
        return jnp.flip(tensor, 0)
    entire_asking_lines = split_attenders(reading_vectors.astype(jnp.float32))
    key_rows = split_attenders(blender_lookup_labels.astype(jnp.float32))
    payload_line_slab = split_attenders(blender_payloads.astype(jnp.float32))
    key_square = lax.optimization_barrier(jnp.sum(key_rows * key_rows, -1, keepdims=True))
    unit_keys = key_rows * lax.rsqrt(key_square + KEY_EPS)
    fading_log_amount = split_attenders(-jnp.exp(-jax.nn.softplus(-fading_logits.astype(jnp.float32)) - 0.5)) + jnp.swapaxes(extra_log_fades, 1, 2)[..., None]
    decays = jnp.exp(fading_log_amount)
    icl_rates = split_attenders(jax.nn.sigmoid(amend_speed_logits.astype(jnp.float32)))
    stored_label_lines = key_rows[None] * icl_rates
    refills = unit_keys[None] * icl_rates
    forward = direction_scan(entire_asking_lines, decays[0], stored_label_lines[0], payload_line_slab, -unit_keys, refills[0])
    backward = flipped(direction_scan(flipped(entire_asking_lines), flipped(decays[1]), flipped(stored_label_lines[1]), flipped(payload_line_slab), flipped(-unit_keys), flipped(refills[1])))
    summed = forward + backward
    center = lax.optimization_barrier(jnp.mean(summed, -1, keepdims=True))
    spread = lax.optimization_barrier(jnp.mean(jnp.square(summed - center), -1, keepdims=True))
    rescaled_lines = (summed - center) * lax.rsqrt(spread + GROUP_EPS) * split_attenders(attender_scaling_vector)
    present_reward_summand = lax.optimization_barrier(jnp.sum(entire_asking_lines * (stored_label_lines[0] + stored_label_lines[1]) * split_attenders(present_reward_factors), -1, keepdims=True)) * payload_line_slab
    merged_attender_lines = ((rescaled_lines + present_reward_summand) * split_attenders(blender_result_valve.astype(jnp.float32))).reshape(STRING_LENGTH, BLENDER_WIDTH)
    merged_attender_lines = merged_attender_lines.astype(jnp.bfloat16)
    group_cols = BLENDER_WIDTH // N_TP
    mixsum = jnp.zeros((STRING_LENGTH, D), jnp.float32)
    for index in range(N_TP):
        partial_mix = jnp.dot(merged_attender_lines[:, index * group_cols:(index + 1) * group_cols], blender_result_projector[index * group_cols:(index + 1) * group_cols], preferred_element_type=jnp.float32)
        mixsum = mixsum + wire_round(partial_mix)
    middle = layer_norm(RESIDUAL_SCALE * skip_stream_entering.astype(jnp.float32) + mixsum, blender_scaling_vector).astype(jnp.bfloat16)
    group_units = FF // N_TP

    def ffn_block(block_rows):
        gate_pre = jnp.dot(block_rows, perceptron_valve_factors, preferred_element_type=jnp.float32)
        up_pre = jnp.dot(block_rows, perceptron_widen_factors, preferred_element_type=jnp.float32)
        inner_act = (jax.nn.silu(gate_pre) * up_pre).astype(jnp.bfloat16)
        downsum = jnp.zeros((block_rows.shape[0], D), jnp.float32)
        for index in range(N_TP):
            partial_down = jnp.dot(inner_act[:, index * group_units:(index + 1) * group_units], perceptron_shrink_factors[index * group_units:(index + 1) * group_units], preferred_element_type=jnp.float32)
            downsum = downsum + wire_round(partial_down)
        return layer_norm(RESIDUAL_SCALE * block_rows.astype(jnp.float32) + downsum, closing_scaling_vector).astype(jnp.bfloat16)
    blocked = lax.map(ffn_block, middle.reshape(STRING_LENGTH // TOK_DEV, TOK_DEV, D))
    return blocked.reshape(STRING_LENGTH, D)
```

```python
import functools
import jax
import jax.numpy as jnp
from jax import lax
from jax.experimental import pallas as pl
from jax.experimental.pallas import tpu as pltpu
from jax.sharding import PartitionSpec as P

RESIDUAL_SCALE = 2.0**0.25
NORM_EPS = 1e-05
GROUP_EPS = 0.00064
KEY_EPS = 1e-06
MESH = pl.DeviceIdType.MESH
VMEM = pl.BlockSpec(memory_space=pltpu.VMEM)
BF = jnp.bfloat16
F32 = jnp.float32


def layer_norm(summand, gain_vec):
    center = jnp.mean(summand, -1, keepdims=True)
    spread = jnp.mean(jnp.square(summand - center), -1, keepdims=True)
    return (summand - center) * lax.rsqrt(spread + NORM_EPS) * gain_vec


def remote(src, dst, send_sem, recv_sem, device):
    return pltpu.make_async_remote_copy(
        src_ref=src,
        dst_ref=dst,
        send_sem=send_sem,
        recv_sem=recv_sem,
        device_id=device,
        device_id_type=MESH,
    )


def greet(devices):
    barrier = pltpu.get_barrier_semaphore()
    for device in devices:
        pl.semaphore_signal(barrier, inc=1, device_id=device, device_id_type=MESH)
    pl.semaphore_wait(barrier, len(devices))


def split_dot(wide, narrow):
    high = wide.astype(BF)
    low = (wide - high.astype(F32)).astype(BF)
    return jnp.dot(high, narrow, preferred_element_type=F32) + jnp.dot(
        low, narrow, preferred_element_type=F32
    )


def recur_kernel(n, pack, vpad, weights, readings, joined, spread, send, recv):
    me = lax.axis_index("sp")
    peers = [lax.rem(me + k, n) for k in range(1, n)]
    greet([{"sp": p} for p in peers])
    copies = [
        remote(weights.at[p], spread.at[me], send.at[k], recv.at[k], {"sp": p})
        for k, p in enumerate(peers)
    ]
    for copy in copies:
        copy.start()
    spread[me] = weights[me]
    blocks, heads, size, _ = pack.shape
    rows = blocks * 8
    wide = 2 * size
    group = 2 if heads % 2 == 0 else 1
    eye = jnp.where(
        lax.broadcasted_iota(jnp.int32, (size, wide), 0) + size
        == lax.broadcasted_iota(jnp.int32, (size, wide), 1),
        1.0,
        0.0,
    ).astype(F32)

    def head_group(hh, carry):
        def block(tb, states):
            states = list(states)
            for i in range(8):
                t = tb * 8 + i
                for g in range(group):
                    h = hh * group + g
                    for d in range(2):
                        row = t if d == 0 else rows - 1 - t
                        vecs = [
                            jnp.broadcast_to(
                                pack[tb, h, :, pl.ds((d * 4 + c) * 8 + i, 1)], (size, wide)
                            )
                            for c in range(4)
                        ]
                        state = states[g * 2 + d]
                        erased = jnp.sum(state * vecs[1], 0, keepdims=True)
                        state = state * vecs[0] + vecs[2] * (
                            vpad[h, pl.ds(row, 1), :] - erased
                        )
                        readings[d, h, pl.ds(row, 1), :] = jnp.sum(
                            state * vecs[3], 0, keepdims=True
                        )
                        states[g * 2 + d] = state
            return tuple(states)

        states = lax.fori_loop(0, blocks, block, (eye,) * (2 * group))
        for g in range(group):
            for d in range(2):
                joined[d * heads + hh * group + g] = states[g * 2 + d].astype(BF)
        return carry

    lax.fori_loop(0, heads // group, head_group, 0)
    for copy in copies:
        copy.wait()


def chain_kernel(n, joined, entering, held, carried, send, recv, send_back, recv_back):
    me = lax.axis_index("sp")
    peers = [lax.rem(me + k, n) for k in range(1, n)]
    greet([{"sp": p} for p in peers])
    copies = [
        remote(joined.at[p], held.at[me], send.at[k], recv.at[k], {"sp": p})
        for k, p in enumerate(peers)
    ]
    for copy in copies:
        copy.start()
    held[me] = joined[me]
    for copy in copies:
        copy.wait()
    size = entering.shape[1]
    back = me // (n // 2)
    state = jnp.zeros((size, size), F32)
    for step in range(n):
        at = back * (n - 1 - step) + (1 - back) * step
        carried[at] = state.astype(BF)
        if step < n - 1:
            block = held[at]
            high = state.astype(BF)
            low = (state - high.astype(F32)).astype(BF)
            move = block[:, size:]
            state = (
                jnp.dot(move, high, preferred_element_type=F32)
                + jnp.dot(move, low, preferred_element_type=F32)
                + block[:, :size].astype(F32)
            )
    copies = [
        remote(carried.at[p], entering.at[me], send_back.at[k], recv_back.at[k], {"sp": p})
        for k, p in enumerate(peers)
    ]
    for copy in copies:
        copy.start()
    entering[me] = carried[me]
    for copy in copies:
        copy.wait()


def places(n1, n2, n_tp):
    sp, tm = lax.axis_index("sp"), lax.axis_index("tp")
    zm, pm = sp // n2, lax.rem(sp, n2)
    along = [{"sp": lax.rem(zm + k, n1) * n2 + pm} for k in range(1, n1)]
    plane = [{"sp": zm * n2 + lax.rem(pm + m, n2)} for m in range(1, n2)]
    across = [{"tp": lax.rem(tm + t, n_tp)} for t in range(1, n_tp)]
    return tm, zm, pm, along, plane, across


def gather_kernel(
    n1,
    n2,
    n_tp,
    readings,
    entering,
    bonus,
    valve,
    gain,
    proj,
    residual,
    scale,
    gathered,
    middle,
    mixed,
    parts,
    landed,
    send_t,
    recv_t,
    send_z,
    recv_z,
    send_p,
    recv_p,
    send_c,
    recv_c,
):
    tm, zm, pm, along, plane, across = places(n1, n2, n_tp)
    greet(along + plane + across)
    heads = readings.shape[1]
    rows = readings.shape[2]
    size = entering.shape[1]
    for h in range(heads):
        cols = slice(h * size, (h + 1) * size)
        total = None
        for d in range(2):
            read = readings[d, h]
            term = read[:, :size] + split_dot(read[:, size:], entering[d * heads + h])
            total = term if total is None else total + term
        center = jnp.mean(total, -1, keepdims=True)
        spread = jnp.mean(jnp.square(total - center), -1, keepdims=True)
        normed = (total - center) * lax.rsqrt(spread + GROUP_EPS) * gain[:, cols]
        mixed[:, cols] = ((normed + bonus[:, cols]) * valve[:, cols].astype(F32)).astype(BF)
    share = rows // n_tp
    product = jnp.dot(mixed[...], proj[...], preferred_element_type=F32).astype(BF)
    for t in range(n_tp):
        parts[t] = product[t * share : (t + 1) * share]
    copies = [
        remote(
            parts.at[lax.rem(tm + t + 1, n_tp)], landed.at[t], send_t.at[t], recv_t.at[t], dev
        )
        for t, dev in enumerate(across)
    ]
    for copy in copies:
        copy.start()
    for copy in copies:
        copy.wait()
    mixsum = parts[tm].astype(F32)
    for t in range(n_tp - 1):
        mixsum = mixsum + landed[t].astype(F32)
    own = layer_norm(RESIDUAL_SCALE * residual[...].astype(F32) + mixsum, scale[...]).astype(BF)
    middle[...] = own
    gathered[tm, zm, pm] = own

    started = []

    def begin(copy):
        copy.start()
        started.append(copy)
        return copy

    def slot(k, m):
        z, p = lax.rem(zm + n1 - k, n1), lax.rem(pm + n2 - m, n2)
        return gathered.at[tm, z, p]

    first = slot(0, 0)
    zs = [
        begin(remote(first, first, send_z.at[k], recv_z.at[k], dev))
        for k, dev in enumerate(along)
    ]

    def to_plane(k):
        return [
            begin(remote(slot(k, 0), slot(k, 0), send_p.at[k, m], recv_p.at[k, m], dev))
            for m, dev in enumerate(plane)
        ]

    def to_cores(k, m):
        for t, dev in enumerate(across):
            begin(
                remote(slot(k, m), slot(k, m), send_c.at[t, k, m], recv_c.at[t, k, m], dev)
            )

    ps = [to_plane(0)]
    to_cores(0, 0)
    for k in range(1, n1):
        zs[k - 1].wait_recv()
        ps.append(to_plane(k))
        to_cores(k, 0)
    for k in range(n1):
        for m in range(1, n2):
            ps[k][m - 1].wait_recv()
            to_cores(k, m)
    plain = set(map(id, zs)) | {id(c) for row in ps for c in row}
    for copy in started:
        copy.wait_send()
        if id(copy) not in plain:
            copy.wait_recv()


def scatter_kernel(
    n1,
    n2,
    n_tp,
    terms,
    middle,
    scale,
    out,
    land_c,
    plane_sum,
    land_p,
    line_sum,
    land_z,
    send_c,
    recv_c,
    send_p,
    recv_p,
    send_z,
    recv_z,
):
    tm, zm, pm, along, plane, across = places(n1, n2, n_tp)
    greet(along + plane + across)
    order = list(range(1, n1)) + [0]
    started = []

    def begin(copy):
        copy.start()
        started.append(copy)
        return copy

    def line(k):
        return lax.rem(zm + k, n1)

    cores = {
        k: [
            begin(
                remote(
                    terms.at[lax.rem(tm + t + 1, n_tp), line(k)],
                    land_c.at[t, k],
                    send_c.at[t, k],
                    recv_c.at[t, k],
                    dev,
                )
            )
            for t, dev in enumerate(across)
        ]
        for k in order
    }
    planes = {}
    for k in order:
        for copy in cores[k]:
            copy.wait_recv()
        for p in range(n2):
            total = terms[tm, line(k), p].astype(F32)
            for t in range(n_tp - 1):
                total = total + land_c[t, k, p].astype(F32)
            plane_sum[k, p] = total.astype(BF)
        planes[k] = [
            begin(
                remote(
                    plane_sum.at[k, lax.rem(pm + m + 1, n2)],
                    land_p.at[k, m],
                    send_p.at[k, m],
                    recv_p.at[k, m],
                    dev,
                )
            )
            for m, dev in enumerate(plane)
        ]
    lines = []
    for k in order:
        for copy in planes[k]:
            copy.wait_recv()
        total = plane_sum[k, pm].astype(F32)
        for m in range(n2 - 1):
            total = total + land_p[k, m].astype(F32)
        if k:
            line_sum[k - 1] = total.astype(BF)
            lines.append(
                begin(
                    remote(
                        line_sum.at[k - 1],
                        land_z.at[k - 1],
                        send_z.at[k - 1],
                        recv_z.at[k - 1],
                        along[k - 1],
                    )
                )
            )
    for k, copy in enumerate(lines):
        copy.wait_recv()
        total = total + land_z[k].astype(F32)
    out[...] = layer_norm(RESIDUAL_SCALE * middle[...].astype(F32) + total, scale[...]).astype(BF)
    for copy in started:
        copy.wait_send()


def params(number):
    return pltpu.CompilerParams(
        collective_id=number, has_side_effects=True, vmem_limit_bytes=60 * 1024 * 1024
    )


def sds(shape, kind):
    return jax.ShapeDtypeStruct(shape, kind)


def chain_gathered(joined, n, heads, size):
    every = lax.all_gather(joined, "sp")
    me = lax.axis_index("sp")

    def walk(half, ahead, backward):
        def one(step, state):
            block = half[n - 1 - step if backward else step].astype(F32)
            return (
                jnp.einsum(
                    "hij,hjk->hik", block[..., size:], state, precision=lax.Precision.HIGHEST
                )
                + block[..., :size]
            )

        return lax.fori_loop(0, ahead, one, jnp.zeros((heads, size, size), F32))

    return jnp.concatenate(
        [walk(every[:, :heads], me, False), walk(every[:, heads:], n - 1 - me, True)], 0
    ).astype(BF)


def shards(
    skip_stream_entering,
    reading_vectors,
    blender_lookup_labels,
    blender_payloads,
    blender_result_valve,
    fading_logits,
    amend_speed_logits,
    extra_log_fades,
    present_reward_factors,
    attender_scaling_vector,
    blender_result_projector,
    blender_scaling_vector,
    perceptron_valve_factors,
    perceptron_widen_factors,
    perceptron_shrink_factors,
    closing_scaling_vector,
):
    n, n_tp = lax.axis_size("sp"), lax.axis_size("tp")
    n1 = 4 if n % 4 == 0 else 1
    n2 = n // n1
    rows, width = reading_vectors.shape
    heads = extra_log_fades.shape[1]
    size = width // heads
    model = skip_stream_entering.shape[1]
    share = rows // n_tp
    dma = pltpu.SemaphoreType.DMA

    def split(tensor):
        return tensor.reshape(tensor.shape[:-1] + (heads, size))

    query = split(reading_vectors.astype(F32))
    key = split(blender_lookup_labels.astype(F32))
    value = split(blender_payloads.astype(F32))
    erase = key / (jnp.sum(key * key, -1, keepdims=True) + KEY_EPS)
    decays = jnp.exp(
        split(-jnp.exp(-jax.nn.softplus(-fading_logits.astype(F32)) - 0.5))
        + jnp.swapaxes(extra_log_fades, 1, 2)[..., None]
    )
    written = key[None] * split(jax.nn.sigmoid(amend_speed_logits.astype(F32)))
    flip = functools.partial(jnp.flip, axis=0)
    pack = jnp.stack(
        [decays[0], erase, written[0], query]
        + [flip(decays[1]), flip(erase), flip(written[1]), flip(query)]
    )
    pack = pack.reshape(8, rows // 8, 8, heads, size).transpose(1, 3, 4, 0, 2)
    pack = pack.reshape(rows // 8, heads, size, 64)
    vpad = jnp.swapaxes(jnp.concatenate([value, jnp.zeros_like(value)], -1), 0, 1)
    bonus = (
        jnp.sum(query * (written[0] + written[1]) * split(present_reward_factors), -1, keepdims=True)
        * value
    ).reshape(rows, width)

    depth = perceptron_valve_factors.shape[0]
    units = perceptron_valve_factors.shape[1] // n
    weights = jnp.stack(
        [
            perceptron_valve_factors.T.reshape(n, units, depth),
            perceptron_widen_factors.T.reshape(n, units, depth),
            perceptron_shrink_factors.reshape(n, units, depth),
        ],
        1,
    )
    readings, joined, spread = pl.pallas_call(
        functools.partial(recur_kernel, n),
        name="recur",
        out_shape=(
            sds((2, heads, rows, 2 * size), F32),
            sds((2 * heads, size, 2 * size), BF),
            sds(weights.shape, BF),
        ),
        in_specs=[VMEM] * 3,
        out_specs=(VMEM,) * 3,
        scratch_shapes=[dma((n - 1,)), dma((n - 1,))],
        compiler_params=params(0),
    )(pack, vpad, weights)

    if 2 * heads == n:
        entering = pl.pallas_call(
            functools.partial(chain_kernel, n),
            name="chain",
            out_shape=sds((n, size, size), BF),
            in_specs=[VMEM],
            out_specs=VMEM,
            scratch_shapes=[
                pltpu.VMEM((n, size, 2 * size), BF),
                pltpu.VMEM((n, size, size), BF),
            ]
            + [dma((n - 1,))] * 4,
            compiler_params=params(1),
        )(joined)
    else:
        entering = chain_gathered(joined, n, heads, size)

    residual = lax.dynamic_slice_in_dim(
        skip_stream_entering, lax.axis_index("tp") * share, share, 0
    )
    gathered, middle = pl.pallas_call(
        functools.partial(gather_kernel, n1, n2, n_tp),
        name="gather",
        out_shape=(sds((n_tp, n1, n2, share, model), BF), sds((share, model), BF)),
        in_specs=[VMEM] * 8,
        out_specs=(VMEM,) * 2,
        scratch_shapes=[
            pltpu.VMEM((rows, width), BF),
            pltpu.VMEM((n_tp, share, model), BF),
            pltpu.VMEM((n_tp - 1, share, model), BF),
            dma((n_tp - 1,)),
            dma((n_tp - 1,)),
            dma((n1 - 1,)),
            dma((n1 - 1,)),
            dma((n1, n2 - 1)),
            dma((n1, n2 - 1)),
            dma((n_tp - 1, n1, n2)),
            dma((n_tp - 1, n1, n2)),
        ],
        compiler_params=params(2),
    )(
        readings,
        entering,
        bonus,
        blender_result_valve,
        attender_scaling_vector[None],
        blender_result_projector,
        residual,
        blender_scaling_vector[None],
    )

    tokens = gathered.reshape(-1, model)
    gate = spread[:, 0].transpose(0, 2, 1).reshape(model, units)
    up = spread[:, 1].transpose(0, 2, 1).reshape(model, units)
    down = spread[:, 2].transpose(1, 0, 2).reshape(units, model)
    inner = (
        jax.nn.silu(jnp.dot(tokens, gate, preferred_element_type=F32))
        * jnp.dot(tokens, up, preferred_element_type=F32)
    ).astype(BF)
    terms = jnp.dot(inner, down, preferred_element_type=F32).astype(BF)

    return pl.pallas_call(
        functools.partial(scatter_kernel, n1, n2, n_tp),
        name="scatter",
        out_shape=sds((share, model), BF),
        in_specs=[VMEM] * 3,
        out_specs=VMEM,
        scratch_shapes=[
            pltpu.VMEM((n_tp - 1, n1, n2, share, model), BF),
            pltpu.VMEM((n1, n2, share, model), BF),
            pltpu.VMEM((n1, n2 - 1, share, model), BF),
            pltpu.VMEM((n1 - 1, share, model), BF),
            pltpu.VMEM((n1 - 1, share, model), BF),
            dma((n_tp - 1, n1)),
            dma((n_tp - 1, n1)),
            dma((n1, n2 - 1)),
            dma((n1, n2 - 1)),
            dma((n1 - 1,)),
            dma((n1 - 1,)),
        ],
        compiler_params=params(3),
    )(terms.reshape(gathered.shape), middle, closing_scaling_vector[None])


def solution(mesh):
    return jax.shard_map(
        shards,
        mesh=mesh,
        in_specs=(
            P("sp", None),
            P("sp", "tp"),
            P("sp", "tp"),
            P("sp", "tp"),
            P("sp", "tp"),
            P(None, "sp", "tp"),
            P(None, "sp", "tp"),
            P(None, "tp", "sp"),
            P("tp"),
            P("tp"),
            P("tp", None),
            P(),
            P("sp", "tp"),
            P("sp", "tp"),
            P("tp", "sp"),
            P(),
        ),
        out_specs=P(("sp", "tp"), None),
        check_vma=False,
    )
```

```python
import functools
import jax
import jax.numpy as jnp
from jax import lax
from jax.experimental import pallas as pl
from jax.experimental.pallas import tpu as pltpu
from jax.sharding import PartitionSpec as P

RESIDUAL_SCALE = 2.0**0.25
NORM_EPS = 1e-05
GROUP_EPS = 0.00064
KEY_EPS = 1e-06
MESH = pl.DeviceIdType.MESH
VMEM = pl.BlockSpec(memory_space=pltpu.VMEM)
BF = jnp.bfloat16
F32 = jnp.float32


def layer_norm(summand, gain_vec):
    center = jnp.mean(summand, -1, keepdims=True)
    spread = jnp.mean(jnp.square(summand - center), -1, keepdims=True)
    return (summand - center) * lax.rsqrt(spread + NORM_EPS) * gain_vec


def remote(src, dst, send_sem, recv_sem, device):
    return pltpu.make_async_remote_copy(
        src_ref=src,
        dst_ref=dst,
        send_sem=send_sem,
        recv_sem=recv_sem,
        device_id=device,
        device_id_type=MESH,
    )


def greet(devices):
    barrier = pltpu.get_barrier_semaphore()
    for device in devices:
        pl.semaphore_signal(barrier, inc=1, device_id=device, device_id_type=MESH)
    pl.semaphore_wait(barrier, len(devices))


def split_dot(wide, narrow):
    high = wide.astype(BF)
    low = (wide - high.astype(F32)).astype(BF)
    return jnp.dot(high, narrow, preferred_element_type=F32) + jnp.dot(
        low, narrow, preferred_element_type=F32
    )


def recur_kernel(n, pack, vpad, weights, readings, joined, spread, send, recv):
    me = lax.axis_index("sp")
    peers = [lax.rem(me + k, n) for k in range(1, n)]
    greet([{"sp": p} for p in peers])
    copies = [
        remote(weights.at[p], spread.at[me], send.at[k], recv.at[k], {"sp": p})
        for k, p in enumerate(peers)
    ]
    for copy in copies:
        copy.start()
    spread[me] = weights[me]
    blocks, heads, size, _ = pack.shape
    rows = blocks * 8
    wide = 2 * size
    group = 2 if heads % 2 == 0 else 1
    eye = jnp.where(
        lax.broadcasted_iota(jnp.int32, (size, wide), 0) + size
        == lax.broadcasted_iota(jnp.int32, (size, wide), 1),
        1.0,
        0.0,
    ).astype(F32)

    def head_group(hh, carry):
        def block(tb, states):
            states = list(states)
            for i in range(8):
                t = tb * 8 + i
                for g in range(group):
                    h = hh * group + g
                    for d in range(2):
                        row = t if d == 0 else rows - 1 - t
                        vecs = [
                            jnp.broadcast_to(
                                pack[tb, h, :, pl.ds((d * 4 + c) * 8 + i, 1)], (size, wide)
                            )
                            for c in range(4)
                        ]
                        state = states[g * 2 + d]
                        erased = jnp.sum(state * vecs[1], 0, keepdims=True)
                        state = state * vecs[0] + vecs[2] * (
                            vpad[h, pl.ds(row, 1), :] - erased
                        )
                        readings[d, h, pl.ds(row, 1), :] = jnp.sum(
                            state * vecs[3], 0, keepdims=True
                        )
                        states[g * 2 + d] = state
            return tuple(states)

        states = lax.fori_loop(0, blocks, block, (eye,) * (2 * group))
        for g in range(group):
            for d in range(2):
                joined[d * heads + hh * group + g] = states[g * 2 + d].astype(BF)
        return carry

    lax.fori_loop(0, heads // group, head_group, 0)
    for copy in copies:
        copy.wait()


def chain_kernel(
    n,
    joined,
    weights,
    entering,
    spread,
    held,
    carried,
    send,
    recv,
    send_back,
    recv_back,
    send_weights,
    recv_weights,
):
    me = lax.axis_index("sp")
    peers = [lax.rem(me + k, n) for k in range(1, n)]
    greet([{"sp": p} for p in peers])
    copies = [
        remote(joined.at[p], held.at[me], send.at[k], recv.at[k], {"sp": p})
        for k, p in enumerate(peers)
    ]
    for copy in copies:
        copy.start()
    held[me] = joined[me]
    for copy in copies:
        copy.wait()
    moves = [
        remote(weights.at[p], spread.at[me], send_weights.at[k], recv_weights.at[k], {"sp": p})
        for k, p in enumerate(peers)
    ]
    for copy in moves:
        copy.start()
    spread[me] = weights[me]
    size = entering.shape[1]
    back = me // (n // 2)
    state = jnp.zeros((size, size), F32)
    for step in range(n):
        at = back * (n - 1 - step) + (1 - back) * step
        carried[at] = state.astype(BF)
        if step < n - 1:
            block = held[at]
            high = state.astype(BF)
            low = (state - high.astype(F32)).astype(BF)
            move = block[:, size:]
            state = (
                jnp.dot(move, high, preferred_element_type=F32)
                + jnp.dot(move, low, preferred_element_type=F32)
                + block[:, :size].astype(F32)
            )
    copies = [
        remote(carried.at[p], entering.at[me], send_back.at[k], recv_back.at[k], {"sp": p})
        for k, p in enumerate(peers)
    ]
    for copy in copies:
        copy.start()
    entering[me] = carried[me]
    for copy in copies + moves:
        copy.wait()


def places(n1, n2, n_tp):
    sp, tm = lax.axis_index("sp"), lax.axis_index("tp")
    zm, pm = sp // n2, lax.rem(sp, n2)
    along = [{"sp": lax.rem(zm + k, n1) * n2 + pm} for k in range(1, n1)]
    plane = [{"sp": zm * n2 + lax.rem(pm + m, n2)} for m in range(1, n2)]
    across = [{"tp": lax.rem(tm + t, n_tp)} for t in range(1, n_tp)]
    return tm, zm, pm, along, plane, across


def gather_kernel(
    n1,
    n2,
    n_tp,
    readings,
    entering,
    bonus,
    valve,
    gain,
    proj,
    residual,
    scale,
    gathered,
    middle,
    mixed,
    parts,
    landed,
    send_t,
    recv_t,
    send_z,
    recv_z,
    send_p,
    recv_p,
    send_c,
    recv_c,
):
    tm, zm, pm, along, plane, across = places(n1, n2, n_tp)
    greet(along + plane + across)
    heads = readings.shape[1]
    rows = readings.shape[2]
    size = entering.shape[1]
    for h in range(heads):
        cols = slice(h * size, (h + 1) * size)
        total = None
        for d in range(2):
            read = readings[d, h]
            term = read[:, :size] + split_dot(read[:, size:], entering[d * heads + h])
            total = term if total is None else total + term
        center = jnp.mean(total, -1, keepdims=True)
        spread = jnp.mean(jnp.square(total - center), -1, keepdims=True)
        normed = (total - center) * lax.rsqrt(spread + GROUP_EPS) * gain[:, cols]
        mixed[:, cols] = ((normed + bonus[:, cols]) * valve[:, cols].astype(F32)).astype(BF)
    share = rows // n_tp
    product = jnp.dot(mixed[...], proj[...], preferred_element_type=F32).astype(BF)
    for t in range(n_tp):
        parts[t] = product[t * share : (t + 1) * share]
    copies = [
        remote(
            parts.at[lax.rem(tm + t + 1, n_tp)], landed.at[t], send_t.at[t], recv_t.at[t], dev
        )
        for t, dev in enumerate(across)
    ]
    for copy in copies:
        copy.start()
    for copy in copies:
        copy.wait()
    mixsum = parts[tm].astype(F32)
    for t in range(n_tp - 1):
        mixsum = mixsum + landed[t].astype(F32)
    own = layer_norm(RESIDUAL_SCALE * residual[...].astype(F32) + mixsum, scale[...]).astype(BF)
    middle[...] = own
    gathered[tm, zm, pm] = own

    started = []

    def begin(copy):
        copy.start()
        started.append(copy)
        return copy

    def slot(k, m):
        z, p = lax.rem(zm + n1 - k, n1), lax.rem(pm + n2 - m, n2)
        return gathered.at[tm, z, p]

    first = slot(0, 0)
    zs = [
        begin(remote(first, first, send_z.at[k], recv_z.at[k], dev))
        for k, dev in enumerate(along)
    ]

    def to_plane(k):
        return [
            begin(remote(slot(k, 0), slot(k, 0), send_p.at[k, m], recv_p.at[k, m], dev))
            for m, dev in enumerate(plane)
        ]

    def to_cores(k, m):
        for t, dev in enumerate(across):
            begin(
                remote(slot(k, m), slot(k, m), send_c.at[t, k, m], recv_c.at[t, k, m], dev)
            )

    ps = [to_plane(0)]
    to_cores(0, 0)
    for k in range(1, n1):
        zs[k - 1].wait_recv()
        ps.append(to_plane(k))
        to_cores(k, 0)
    for k in range(n1):
        for m in range(1, n2):
            ps[k][m - 1].wait_recv()
            to_cores(k, m)
    plain = set(map(id, zs)) | {id(c) for row in ps for c in row}
    for copy in started:
        copy.wait_send()
        if id(copy) not in plain:
            copy.wait_recv()


def scatter_kernel(
    n1,
    n2,
    n_tp,
    terms,
    middle,
    scale,
    out,
    land_c,
    plane_sum,
    land_p,
    line_sum,
    land_z,
    send_c,
    recv_c,
    send_p,
    recv_p,
    send_z,
    recv_z,
):
    tm, zm, pm, along, plane, across = places(n1, n2, n_tp)
    greet(along + plane + across)
    order = list(range(1, n1)) + [0]
    started = []

    def begin(copy):
        copy.start()
        started.append(copy)
        return copy

    def line(k):
        return lax.rem(zm + k, n1)

    cores = {
        k: [
            begin(
                remote(
                    terms.at[lax.rem(tm + t + 1, n_tp), line(k)],
                    land_c.at[t, k],
                    send_c.at[t, k],
                    recv_c.at[t, k],
                    dev,
                )
            )
            for t, dev in enumerate(across)
        ]
        for k in order
    }
    planes = {}
    for k in order:
        for copy in cores[k]:
            copy.wait_recv()
        for p in range(n2):
            total = terms[tm, line(k), p].astype(F32)
            for t in range(n_tp - 1):
                total = total + land_c[t, k, p].astype(F32)
            plane_sum[k, p] = total.astype(BF)
        planes[k] = [
            begin(
                remote(
                    plane_sum.at[k, lax.rem(pm + m + 1, n2)],
                    land_p.at[k, m],
                    send_p.at[k, m],
                    recv_p.at[k, m],
                    dev,
                )
            )
            for m, dev in enumerate(plane)
        ]
    lines = []
    for k in order:
        for copy in planes[k]:
            copy.wait_recv()
        total = plane_sum[k, pm].astype(F32)
        for m in range(n2 - 1):
            total = total + land_p[k, m].astype(F32)
        if k:
            line_sum[k - 1] = total.astype(BF)
            lines.append(
                begin(
                    remote(
                        line_sum.at[k - 1],
                        land_z.at[k - 1],
                        send_z.at[k - 1],
                        recv_z.at[k - 1],
                        along[k - 1],
                    )
                )
            )
    for k, copy in enumerate(lines):
        copy.wait_recv()
        total = total + land_z[k].astype(F32)
    out[...] = layer_norm(RESIDUAL_SCALE * middle[...].astype(F32) + total, scale[...]).astype(BF)
    for copy in started:
        copy.wait_send()


def params(number):
    return pltpu.CompilerParams(
        collective_id=number, has_side_effects=True, vmem_limit_bytes=60 * 1024 * 1024
    )


def sds(shape, kind):
    return jax.ShapeDtypeStruct(shape, kind)


def chain_gathered(joined, n, heads, size):
    every = lax.all_gather(joined, "sp")
    me = lax.axis_index("sp")

    def walk(half, ahead, backward):
        def one(step, state):
            block = half[n - 1 - step if backward else step].astype(F32)
            return (
                jnp.einsum(
                    "hij,hjk->hik", block[..., size:], state, precision=lax.Precision.HIGHEST
                )
                + block[..., :size]
            )

        return lax.fori_loop(0, ahead, one, jnp.zeros((heads, size, size), F32))

    return jnp.concatenate(
        [walk(every[:, :heads], me, False), walk(every[:, heads:], n - 1 - me, True)], 0
    ).astype(BF)


def shards(
    skip_stream_entering,
    reading_vectors,
    blender_lookup_labels,
    blender_payloads,
    blender_result_valve,
    fading_logits,
    amend_speed_logits,
    extra_log_fades,
    present_reward_factors,
    attender_scaling_vector,
    blender_result_projector,
    blender_scaling_vector,
    perceptron_valve_factors,
    perceptron_widen_factors,
    perceptron_shrink_factors,
    closing_scaling_vector,
):
    n, n_tp = lax.axis_size("sp"), lax.axis_size("tp")
    n1 = 4 if n % 4 == 0 else 1
    n2 = n // n1
    rows, width = reading_vectors.shape
    heads = extra_log_fades.shape[1]
    size = width // heads
    model = skip_stream_entering.shape[1]
    share = rows // n_tp
    dma = pltpu.SemaphoreType.DMA

    def split(tensor):
        return tensor.reshape(tensor.shape[:-1] + (heads, size))

    query = split(reading_vectors.astype(F32))
    key = split(blender_lookup_labels.astype(F32))
    value = split(blender_payloads.astype(F32))
    erase = key / (jnp.sum(key * key, -1, keepdims=True) + KEY_EPS)
    decays = jnp.exp(
        split(-jnp.exp(-jax.nn.softplus(-fading_logits.astype(F32)) - 0.5))
        + jnp.swapaxes(extra_log_fades, 1, 2)[..., None]
    )
    written = key[None] * split(jax.nn.sigmoid(amend_speed_logits.astype(F32)))
    flip = functools.partial(jnp.flip, axis=0)
    pack = jnp.stack(
        [decays[0], erase, written[0], query]
        + [flip(decays[1]), flip(erase), flip(written[1]), flip(query)]
    )
    pack = pack.reshape(8, rows // 8, 8, heads, size).transpose(1, 3, 4, 0, 2)
    pack = pack.reshape(rows // 8, heads, size, 64)
    vpad = jnp.swapaxes(jnp.concatenate([value, jnp.zeros_like(value)], -1), 0, 1)
    bonus = (
        jnp.sum(query * (written[0] + written[1]) * split(present_reward_factors), -1, keepdims=True)
        * value
    ).reshape(rows, width)

    depth = perceptron_valve_factors.shape[0]
    units = perceptron_valve_factors.shape[1] // n
    owners = 2 * heads == n
    shrink = perceptron_shrink_factors.reshape(n, units, depth)
    weights = jnp.stack(
        [
            perceptron_valve_factors.T.reshape(n, units, depth),
            perceptron_widen_factors.T.reshape(n, units, depth),
        ]
        + ([] if owners else [shrink]),
        1,
    )
    readings, joined, spread = pl.pallas_call(
        functools.partial(recur_kernel, n),
        name="recur",
        out_shape=(
            sds((2, heads, rows, 2 * size), F32),
            sds((2 * heads, size, 2 * size), BF),
            sds(weights.shape, BF),
        ),
        in_specs=[VMEM] * 3,
        out_specs=(VMEM,) * 3,
        scratch_shapes=[dma((n - 1,)), dma((n - 1,))],
        compiler_params=params(0),
    )(pack, vpad, weights)

    if owners:
        entering, narrow = pl.pallas_call(
            functools.partial(chain_kernel, n),
            name="chain",
            out_shape=(sds((n, size, size), BF), sds(shrink.shape, BF)),
            in_specs=[VMEM] * 2,
            out_specs=(VMEM,) * 2,
            scratch_shapes=[
                pltpu.VMEM((n, size, 2 * size), BF),
                pltpu.VMEM((n, size, size), BF),
            ]
            + [dma((n - 1,))] * 6,
            compiler_params=params(1),
        )(joined, shrink)
    else:
        entering = chain_gathered(joined, n, heads, size)
        narrow = spread[:, 2]

    residual = lax.dynamic_slice_in_dim(
        skip_stream_entering, lax.axis_index("tp") * share, share, 0
    )
    gathered, middle = pl.pallas_call(
        functools.partial(gather_kernel, n1, n2, n_tp),
        name="gather",
        out_shape=(sds((n_tp, n1, n2, share, model), BF), sds((share, model), BF)),
        in_specs=[VMEM] * 8,
        out_specs=(VMEM,) * 2,
        scratch_shapes=[
            pltpu.VMEM((rows, width), BF),
            pltpu.VMEM((n_tp, share, model), BF),
            pltpu.VMEM((n_tp - 1, share, model), BF),
            dma((n_tp - 1,)),
            dma((n_tp - 1,)),
            dma((n1 - 1,)),
            dma((n1 - 1,)),
            dma((n1, n2 - 1)),
            dma((n1, n2 - 1)),
            dma((n_tp - 1, n1, n2)),
            dma((n_tp - 1, n1, n2)),
        ],
        compiler_params=params(2),
    )(
        readings,
        entering,
        bonus,
        blender_result_valve,
        attender_scaling_vector[None],
        blender_result_projector,
        residual,
        blender_scaling_vector[None],
    )

    tokens = gathered.reshape(-1, model)
    gate = spread[:, 0].transpose(0, 2, 1).reshape(model, units)
    up = spread[:, 1].transpose(0, 2, 1).reshape(model, units)
    down = narrow.transpose(1, 0, 2).reshape(units, model)
    inner = (
        jax.nn.silu(jnp.dot(tokens, gate, preferred_element_type=F32))
        * jnp.dot(tokens, up, preferred_element_type=F32)
    ).astype(BF)
    terms = jnp.dot(inner, down, preferred_element_type=F32).astype(BF)

    return pl.pallas_call(
        functools.partial(scatter_kernel, n1, n2, n_tp),
        name="scatter",
        out_shape=sds((share, model), BF),
        in_specs=[VMEM] * 3,
        out_specs=VMEM,
        scratch_shapes=[
            pltpu.VMEM((n_tp - 1, n1, n2, share, model), BF),
            pltpu.VMEM((n1, n2, share, model), BF),
            pltpu.VMEM((n1, n2 - 1, share, model), BF),
            pltpu.VMEM((n1 - 1, share, model), BF),
            pltpu.VMEM((n1 - 1, share, model), BF),
            dma((n_tp - 1, n1)),
            dma((n_tp - 1, n1)),
            dma((n1, n2 - 1)),
            dma((n1, n2 - 1)),
            dma((n1 - 1,)),
            dma((n1 - 1,)),
        ],
        compiler_params=params(3),
    )(terms.reshape(gathered.shape), middle, closing_scaling_vector[None])


def solution(mesh):
    return jax.shard_map(
        shards,
        mesh=mesh,
        in_specs=(
            P("sp", None),
            P("sp", "tp"),
            P("sp", "tp"),
            P("sp", "tp"),
            P("sp", "tp"),
            P(None, "sp", "tp"),
            P(None, "sp", "tp"),
            P(None, "tp", "sp"),
            P("tp"),
            P("tp"),
            P("tp", None),
            P(),
            P("sp", "tp"),
            P("sp", "tp"),
            P("tp", "sp"),
            P(),
        ),
        out_specs=P(("sp", "tp"), None),
        check_vma=False,
    )
```
